32 devices in a mesh: ep: 8 (over z, x), tp: 4 (over y, core).
Axes of the slice: x: 2, y: 2, z: 4, core: 2. Of those that a mesh axis runs over, the one named last changes fastest.
Arguments:
- mix_input: bfloat16 [3072, 2048], P('ep', 'tp'), may hold values from -6 to 6
- mix_gain: float32 [2048], replicated, may hold values from 0.1 to 1.9
- gate_b_weight: bfloat16 [2048, 2048], P(None, 'tp'), may hold values from -0.125 to 0.125
- gate_c_weight: bfloat16 [2048, 2048], P(None, 'tp'), may hold values from -0.125 to 0.125
- value_weight: bfloat16 [2048, 2048], P(None, 'tp'), may hold values from -0.125 to 0.125
- conv_weight: float32 [3, 2048], P(None, 'tp'), may hold values from -3 to 3
- out_weight: bfloat16 [2048, 2048], P('tp'), may hold values from -0.125 to 0.125
- expert_input: bfloat16 [1280, 2048], P('ep', 'tp'), may hold values from -6 to 6
- expert_gain: float32 [2048], replicated, may hold values from 0.1 to 1.9
- routes: int32 [1280, 2], P('ep'), may hold values from 0 to 7, all different within a row; in each aligned block of 160 rows (0 to 159, 160 to 319, ...) at most 80 rows name the same one
- route_weight: float32 [1280, 2], P('ep'), may hold values from 0.2 to 1
- expert_gate: bfloat16 [8, 2048, 3072], P('ep', None, 'tp'), may hold values from -0.125 to 0.125
- expert_up: bfloat16 [8, 2048, 3072], P('ep', None, 'tp'), may hold values from -0.125 to 0.125
- expert_down: bfloat16 [8, 3072, 2048], P('ep', 'tp'), may hold values from -0.109375 to 0.109375
Outputs:
- mix_output: bfloat16 [3072, 2048], P('ep', 'tp')
- expert_output: bfloat16 [1280, 2048], P('ep', 'tp')
The draws below stay inside these ranges and needn't reach their ends.
Inputs may be any that keep to these rules, and one draw needn't show every extreme that they name: `routes`: the 2 experts of a row differ. Among the rows of one device no expert is named more than 80 times, a bound that some block reaches.
All inputs are finite; a program needn't handle non-finite values.
Results may differ from the reference program's by a relative error of at most 0.019.
Values may be sent and summed in bfloat16 or wider, within the bound.
No kernel may reach another device: no remote copies, remote signals or barrier semaphores. Data moves between devices by JAX's collectives and lax.ppermute only.
A program may use at most 64 MiB of HBM per device.

```python
import math
import jax
import jax.numpy as jnp
import numpy as np
from jax import lax

D = 2048
FF = 3072
TOPK = 2
TOK_B = 160
EXPERTS = 8
CAP = 80
TOKENS_A = 3072
TOKENS_B = 1280
N_EP = 8
N_TP = 4


def levels(own_key, dims, split, low, high):
    def one(position, parts):
        draws = jax.random.uniform(jax.random.fold_in(jax.random.fold_in(own_key, 6), position), (parts,), jnp.float32, low / len(split), high / len(split))
        return jnp.repeat(jnp.exp(draws), dims[position] // parts).reshape((-1,) + (1,) * (len(dims) - position - 1))

    factor_of = one(*split[0])
    for cut in split[1:]:
        factor_of = factor_of * one(*cut)
    return factor_of


def shared_out(stream_key, own, number, rows, count, top, bound, slope):
    ranking = jax.random.permutation(stream_key, count)
    packed, common = load_shares(count, rows * top, bound, slope, True), load_shares(count, rows * top, bound, slope, False)
    places = jnp.arange(count)

    def named(tallies, rotation):
        used = int((tallies > 0).sum())
        fixed = max(1, used // 4)
        passed = fixed + (places - fixed + rotation * (used - fixed)) % max(1, count - fixed)
        return jnp.zeros((count,), jnp.int32).at[ranking[jnp.where(places < fixed, places, passed)]].set(jnp.asarray(tallies, jnp.int32))

    tallies = jnp.where(number % 4 == 0, named(packed, number // 4), named(common, number - number // 4 - 1))
    mixed = jax.random.permutation(jax.random.fold_in(own, 3), count)
    donor, receiver = mixed[0:count // 2 * 2:2], mixed[1:count // 2 * 2:2]
    margin = jnp.minimum(tallies[donor] - 1, bound - tallies[receiver]) // 2
    margin = jnp.where((donor == ranking[0]) | (receiver == ranking[0]) | (tallies[receiver] == 0), 0, jnp.maximum(margin, 0))
    passed = jax.random.randint(jax.random.fold_in(own, 4), (count // 2,), 0, 1 << 20) % (margin + 1)
    tallies = tallies.at[donor].add(-passed).at[receiver].add(passed)
    members = jnp.searchsorted(jnp.cumsum(tallies), jnp.arange(rows * top), side="right").astype(jnp.int32)
    listing = members.reshape(top, rows).T
    listing = listing[jax.random.permutation(jax.random.fold_in(own, 1), rows)]
    rotation = jax.random.randint(jax.random.fold_in(own, 2), (rows, 1), 0, top)
    return jnp.take_along_axis(listing, (jnp.arange(top)[None, :] + rotation) % top, axis=1)


def load_shares(number_of, total, bound, slope, full):
    weights = [(1 << 20) // math.isqrt(standing ** slope) + 1 for standing in range(1, number_of + 1)]
    largest = bound if full else min(bound, max(-(-total // number_of), total * weights[0] // sum(weights)))
    least = 1 if total - largest >= number_of - 1 else 0
    counts, rest = [largest] + [least] * (number_of - 1), total - largest - least * (number_of - 1)
    while rest > 0:
        candidates = [i for i in range(1, number_of) if counts[i] < largest] or [i for i in range(1, number_of) if counts[i] < bound]
        mass, left = sum([weights[i] for i in candidates]), rest
        for i in candidates:
            more = min(bound - counts[i], max(1, left * weights[i] // mass), rest)
            counts[i] = counts[i] + more
            rest = rest - more
    return np.array(counts)


def centred(own_key, shape, scale, reach, pieces=(), kind=jnp.bfloat16):
    drawn = scale * jax.random.normal(own_key, shape, jnp.float32)
    if pieces:
        drawn = drawn * levels(own_key, shape, pieces, -0.22, 0.18)
    return jnp.clip(drawn, -reach, reach).astype(kind)


def setup_inputs(seed: int = 0) -> dict:
    splits = jax.random.split(jax.random.key(seed), 15)
    mix_input = centred(splits[0], (TOKENS_A, D), 1.0, 6.0, ((0, 8), (1, 4)))
    mix_gain = jnp.clip(1.0 + 0.18 * jax.random.normal(splits[1], (D,), jnp.float32), 0.1, 1.9)
    gate_b_weight = centred(splits[2], (D, D), D ** -0.5, 0.125, ((1, 4),))
    gate_c_weight = centred(splits[3], (D, D), D ** -0.5, 0.125, ((1, 4),))
    value_weight = centred(splits[4], (D, D), D ** -0.5, 0.125, ((1, 4),))
    conv_weight = centred(splits[5], (3, D), 0.6, 3.0, ((1, 4),), jnp.float32)
    out_weight = centred(splits[6], (D, D), D ** -0.5, 0.125, ((0, 4),))
    expert_input = centred(splits[7], (TOKENS_B, D), 1.0, 6.0, ((0, 8), (1, 4)))
    expert_gain = jnp.clip(1.0 + 0.18 * jax.random.normal(splits[8], (D,), jnp.float32), 0.1, 1.9)
    routes_keys = jax.random.split(jax.random.fold_in(splits[9], 1), TOKENS_B // TOK_B)
    routes_turns = jax.random.permutation(jax.random.fold_in(splits[9], 3), TOKENS_B // TOK_B)
    routes = jax.vmap(lambda own, number: shared_out(jax.random.fold_in(splits[9], 2), own, number, TOK_B, EXPERTS, TOPK, CAP, 1))(routes_keys, routes_turns).reshape((TOKENS_B, TOPK))
    route_weight = jnp.clip(jnp.exp(math.log(1.0) - 1.609438 * jax.random.uniform(splits[10], (TOKENS_B, TOPK), jnp.float32) ** levels(splits[10], (TOKENS_B, TOPK), ((0, 8),), -0.2, 0.2)), 0.2, 1.0)
    expert_gate = centred(splits[11], (EXPERTS, D, FF), D ** -0.5, 0.125, ((0, 8), (2, 4)))
    expert_up = centred(splits[12], (EXPERTS, D, FF), D ** -0.5, 0.125, ((0, 8), (2, 4)))
    expert_down = centred(splits[13], (EXPERTS, FF, D), FF ** -0.5, 0.109375, ((0, 8), (1, 4)))
    return {"mix_input": mix_input, "mix_gain": mix_gain, "gate_b_weight": gate_b_weight, "gate_c_weight": gate_c_weight, "value_weight": value_weight, "conv_weight": conv_weight, "out_weight": out_weight, "expert_input": expert_input, "expert_gain": expert_gain, "routes": routes, "route_weight": route_weight, "expert_gate": expert_gate, "expert_up": expert_up, "expert_down": expert_down}


epsilon = 1e-06
routed_scale = 2.5

def norm_project(source, gain_vector, matrices):
    widened = source.astype(jnp.float32)
    factor = lax.rsqrt(lax.optimization_barrier(jnp.mean(widened * widened, axis=-1, keepdims=True)) + epsilon)
    scaled = (widened * gain_vector).astype(jnp.bfloat16)
    return [jnp.dot(scaled, matrix, preferred_element_type=jnp.float32) * factor for matrix in matrices]

def block_sum(operand, weights):
    span_size = operand.shape[1] // N_TP
    running = jnp.zeros((operand.shape[0], weights.shape[1]), jnp.float32)
    for block_index in range(N_TP):
        low = block_index * span_size
        partial_value = jnp.dot(operand[:, low:low + span_size], weights[low:low + span_size], preferred_element_type=jnp.float32)
        running = running + partial_value.astype(jnp.bfloat16).astype(jnp.float32)
    return running.astype(jnp.bfloat16)

def reference(mix_input, mix_gain, gate_b_weight, gate_c_weight, value_weight, conv_weight, out_weight, expert_input, expert_gain, routes, route_weight, expert_gate, expert_up, expert_down):
    outer_gate, inner_gate, conv_values = norm_project(mix_input, mix_gain, (gate_b_weight, gate_c_weight, value_weight))
    product = inner_gate * conv_values
    seq_length = product.shape[0]
    padded = jnp.concatenate([jnp.zeros((2, product.shape[1]), jnp.float32), product], axis=0)
    convolved = conv_weight[0] * padded[:seq_length] + conv_weight[1] * padded[1:seq_length + 1] + conv_weight[2] * padded[2:]
    gated = (outer_gate * convolved).astype(jnp.bfloat16)
    mix_output = block_sum(gated, out_weight)
    flat_routes = routes.reshape(-1).astype(jnp.int32)
    pair_count = flat_routes.shape[0]
    slot_count = N_EP * CAP
    expert_ids = jnp.arange(EXPERTS, dtype=jnp.int32)
    matches = (flat_routes[:, None] == expert_ids[None, :]).astype(jnp.int32)
    ranks = lax.optimization_barrier(jnp.sum((jnp.cumsum(matches, axis=0) - matches) * matches, axis=1)).astype(jnp.int32)
    owners_all = (jnp.arange(pair_count, dtype=jnp.int32) // TOPK).astype(jnp.int32)

    def one_expert(inputs):
        gate_matrix, up_matrix, down_matrix, expert_id = inputs
        chosen = flat_routes == expert_id
        target = jnp.where(chosen, ranks, slot_count).astype(jnp.int32)
        owners = jnp.zeros((slot_count,), jnp.int32).at[target].set(owners_all, mode='drop')
        gathered = expert_input[owners]
        hidden_gate, hidden_up = norm_project(gathered, expert_gain, (gate_matrix, up_matrix))
        activated = (jax.nn.silu(hidden_gate) * hidden_up).astype(jnp.bfloat16)
        return block_sum(activated, down_matrix)
    results = lax.map(one_expert, (expert_gate, expert_up, expert_down, expert_ids))
    picked = results[flat_routes, ranks].astype(jnp.float32).reshape(routes.shape[0], TOPK, -1)
    normalized = route_weight / lax.optimization_barrier(jnp.sum(route_weight, axis=1, keepdims=True)) * routed_scale
    expert_output = lax.optimization_barrier(jnp.sum(picked * normalized[:, :, None], axis=1)).astype(jnp.bfloat16)
    return (mix_output, expert_output)
```

```python
import jax
import jax.numpy as jnp
from jax import lax
from jax.experimental import pallas as pl
from jax.experimental.pallas import tpu as pltpu
from jax.sharding import PartitionSpec as P

epsilon = 1e-06
routed_scale = 2.5


def passed_along(block, axis, distance):
    devices = range(lax.axis_size(axis))
    route = [(i - distance, i) for i in devices if i - distance in devices]
    return lax.ppermute(block, axis, route)


def swapped(block, axis, mask):
    return lax.ppermute(block, axis, [(i, i ^ mask) for i in range(lax.axis_size(axis))])


def spread(own):
    chips = lax.axis_size("tp") // 2
    mine = [own] + [swapped(own, "tp", 2 * s) for s in range(1, chips)]
    return mine, [swapped(block, "tp", 1) for block in mine]


def dot32(a, b):
    return jnp.dot(a, b, preferred_element_type=jnp.float32)


def column_start(place, distance, side, columns):
    chip = (place // 2) ^ distance
    return pl.multiple_of((2 * chip + (place % 2 if side == 0 else 1 - place % 2)) * columns, columns)


def assemble(place, mine, other, gain, scaled, factor):
    columns = mine[0].shape[1]
    squares = jnp.zeros(factor.shape, jnp.float32)
    for side, refs in enumerate((mine, other)):
        for distance, ref in enumerate(refs):
            at = pl.ds(column_start(place, distance, side, columns), columns)
            widened = ref[...].astype(jnp.float32)
            squares = squares + jnp.sum(widened * widened, axis=1, keepdims=True)
            scaled[:, at] = (widened * gain[:, at]).astype(jnp.bfloat16)
    factor[...] = lax.rsqrt(squares / scaled.shape[1] + epsilon)


def step_of(size):
    return 256 if size % 256 == 0 else size


def whole(shape):
    return pl.BlockSpec(shape, lambda *_: (0,) * len(shape))


def place_spec():
    return pl.BlockSpec(memory_space=pltpu.SMEM)


def expert_kernel(chips, place_ref, *refs):
    mine, other = refs[:chips], refs[chips : 2 * chips]
    gain, gate, up, down, keep, leave, scaled, factor, total = refs[2 * chips :]
    place = place_ref[0]
    step = pl.program_id(0)

    @pl.when(step == 0)
    def _():
        assemble(place, mine, other, gain, scaled, factor)

    hidden_gate = dot32(scaled[...], gate[0]) * factor[...]
    hidden_up = dot32(scaled[...], up[0]) * factor[...]
    activated = (hidden_gate / (1.0 + jnp.exp(-hidden_gate)) * hidden_up).astype(jnp.bfloat16)
    part = dot32(activated, down[0])

    @pl.when(step == 0)
    def _():
        total[...] = part

    @pl.when(step > 0)
    def _():
        total[...] += part

    @pl.when(step == pl.num_programs(0) - 1)
    def _():
        columns = keep.shape[2]
        for distance in range(chips):
            for side, out in enumerate((keep, leave)):
                at = pl.ds(column_start(place, distance, side, columns), columns)
                out[distance] = total[:, at].astype(jnp.bfloat16)


def expert_call(place, mine, other, gain, gate, up, down):
    chips = len(mine)
    rows, columns = mine[0].shape
    width, hidden = gate.shape[1:]
    step = step_of(hidden)
    out = jax.ShapeDtypeStruct((chips, rows, columns), jnp.bfloat16)
    return pl.pallas_call(
        lambda *refs: expert_kernel(chips, *refs),
        grid=(hidden // step,),
        in_specs=[place_spec()]
        + [whole((rows, columns))] * (2 * chips)
        + [
            whole((1, width)),
            pl.BlockSpec((1, width, step), lambda i: (0, 0, i)),
            pl.BlockSpec((1, width, step), lambda i: (0, 0, i)),
            pl.BlockSpec((1, step, width), lambda i: (0, i, 0)),
        ],
        out_specs=[whole(out.shape)] * 2,
        out_shape=[out] * 2,
        scratch_shapes=[
            pltpu.VMEM((rows, width), jnp.bfloat16),
            pltpu.VMEM((rows, 1), jnp.float32),
            pltpu.VMEM((rows, width), jnp.float32),
        ],
        cost_estimate=pl.CostEstimate(
            flops=6 * rows * width * hidden,
            bytes_accessed=6 * width * hidden,
            transcendentals=rows * hidden,
        ),
        name="expert_rows",
    )(place, *mine, *other, gain[None], gate, up, down)


def mixer_kernel(chips, place_ref, *refs):
    mine, other = refs[:chips], refs[chips : 2 * chips]
    gain, gate_b, gate_c, value, product, outer, scaled, factor = refs[2 * chips :]

    @pl.when(pl.program_id(0) == 0)
    def _():
        assemble(place_ref[0], mine, other, gain, scaled, factor)

    rows = scaled[...]
    product[...] = dot32(rows, gate_c[...]) * factor[...] * (dot32(rows, value[...]) * factor[...])
    outer[...] = dot32(rows, gate_b[...]) * factor[...]


def mixer_call(place, mine, other, gain, gate_b, gate_c, value):
    chips = len(mine)
    rows, columns = mine[0].shape
    width = gate_b.shape[0]
    step = step_of(columns)
    out = jax.ShapeDtypeStruct((rows, columns), jnp.float32)
    return pl.pallas_call(
        lambda *refs: mixer_kernel(chips, *refs),
        grid=(columns // step,),
        in_specs=[place_spec()]
        + [whole((rows, columns))] * (2 * chips)
        + [whole((1, width))]
        + [pl.BlockSpec((width, step), lambda i: (0, i))] * 3,
        out_specs=[pl.BlockSpec((rows, step), lambda i: (0, i))] * 2,
        out_shape=[out] * 2,
        scratch_shapes=[
            pltpu.VMEM((rows, width), jnp.bfloat16),
            pltpu.VMEM((rows, 1), jnp.float32),
        ],
        cost_estimate=pl.CostEstimate(
            flops=6 * rows * width * columns, bytes_accessed=6 * width * columns, transcendentals=0
        ),
        name="mixer_rows",
    )(place, *mine, *other, gain[None], gate_b, gate_c, value)


def output_kernel(chips, place_ref, edge, product, outer, taps, weight, keep, leave):
    place = place_ref[0]
    now = product[...]
    row = lax.broadcasted_iota(jnp.int32, now.shape, 0)
    before = jnp.where(row == 0, edge[1:2], pltpu.roll(now, 1, 0))
    earlier = jnp.where(row == 0, edge[0:1], jnp.where(row == 1, edge[1:2], pltpu.roll(now, 2, 0)))
    convolved = taps[0:1] * earlier + taps[1:2] * before + taps[2:3] * now
    gated = (outer[...] * convolved).astype(jnp.bfloat16)
    columns = keep.shape[2]
    for distance in range(chips):
        for side, out in enumerate((keep, leave)):
            at = pl.ds(column_start(place, distance, side, columns), columns)
            out[distance] = dot32(gated, weight[:, at]).astype(jnp.bfloat16)


def output_call(chips, place, edge, product, outer, taps, weight):
    rows, columns = product.shape
    out = jax.ShapeDtypeStruct((chips, rows, columns), jnp.bfloat16)
    return pl.pallas_call(
        lambda *refs: output_kernel(chips, *refs),
        in_specs=[place_spec()] + [pl.BlockSpec(memory_space=pltpu.VMEM)] * 5,
        out_specs=[pl.BlockSpec(memory_space=pltpu.VMEM)] * 2,
        out_shape=[out] * 2,
        cost_estimate=pl.CostEstimate(
            flops=2 * rows * weight.shape[0] * weight.shape[1],
            bytes_accessed=2 * weight.shape[0] * weight.shape[1],
            transcendentals=0,
        ),
        name="mixer_output",
    )(place, edge, product, outer, taps, weight)


def joined(blocks):
    rows, columns = blocks[0].shape
    if rows % 16:
        return jnp.concatenate(blocks, axis=0)

    def kernel(*refs):
        for j, ref in enumerate(refs[:-1]):
            refs[-1][j * rows : (j + 1) * rows] = ref[...]

    return pl.pallas_call(
        kernel,
        in_specs=[pl.BlockSpec(memory_space=pltpu.VMEM)] * len(blocks),
        out_specs=pl.BlockSpec(memory_space=pltpu.VMEM),
        out_shape=jax.ShapeDtypeStruct((rows * len(blocks), columns), blocks[0].dtype),
        name="join_rows",
    )(*blocks)


def scattered(keep, leave, tag):
    with jax.named_scope("core" + tag):
        got = swapped(leave, "tp", 1)
    wide = [keep[s].astype(jnp.float32) + got[s].astype(jnp.float32) for s in range(keep.shape[0])]
    total = wide[0]
    for s in range(1, len(wide)):
        with jax.named_scope("chip" + tag):
            received = swapped(wide[s].astype(jnp.bfloat16), "tp", 2 * s)
        total = total + received.astype(jnp.float32)
    return total.astype(jnp.bfloat16)


def local(
    mix_input,
    mix_gain,
    gate_b_weight,
    gate_c_weight,
    value_weight,
    conv_weight,
    out_weight,
    expert_input,
    expert_gain,
    routes,
    route_weight,
    expert_gate,
    expert_up,
    expert_down,
):
    ep_count = lax.axis_size("ep")
    ep_me = lax.axis_index("ep")
    local_experts = expert_gate.shape[0]
    assert local_experts == 1
    expert_count = local_experts * ep_count
    tok_local, top_count = routes.shape
    capacity = 2 * tok_local * top_count // expert_count
    columns = expert_input.shape[1]
    mix_rows = mix_input.shape[0]
    block_rows = local_experts * capacity
    slots = ep_count * block_rows
    half = ep_count // 2

    place = lax.axis_index("tp").astype(jnp.int32)[None]
    mix_mine, mix_other = spread(mix_input)

    named = [routes[:, k][:, None] for k in range(top_count)]
    experts_iota = lax.broadcasted_iota(jnp.int32, (tok_local, expert_count), 1)
    hits = [(n == experts_iota) for n in named]
    any_hit = hits[0]
    for h in hits[1:]:
        any_hit = any_hit | h
    earlier = (
        lax.broadcasted_iota(jnp.int32, (tok_local, tok_local), 0)
        > lax.broadcasted_iota(jnp.int32, (tok_local, tok_local), 1)
    ).astype(jnp.bfloat16)
    counts = dot32(earlier, any_hit.astype(jnp.bfloat16)).astype(jnp.int32)
    slot_iota = lax.broadcasted_iota(jnp.int32, (tok_local, slots), 1)
    picks = []
    for n, h in zip(named, hits):
        rank = jnp.sum(jnp.where(h, counts, 0), axis=1, keepdims=True)
        index = (n // local_experts ^ ep_me) * block_rows + n % local_experts * capacity + rank
        picks.append(slot_iota == index)
    send = picks[0]
    for p in picks[1:]:
        send = send | p
    outgoing = lax.dot_general(
        send.astype(jnp.bfloat16),
        expert_input,
        (((0,), (0,)), ((), ())),
        preferred_element_type=jnp.float32,
    ).astype(jnp.bfloat16)
    outgoing = outgoing.reshape(ep_count, block_rows, columns)

    chunks = [range(half, ep_count), range(half)] if half else [range(ep_count)]
    arrived = []
    for members in chunks:
        arrived.append([swapped(outgoing[s], "ep", s) if s else outgoing[0] for s in members])

    product, outer_gate = mixer_call(
        place, mix_mine, mix_other, mix_gain, gate_b_weight, gate_c_weight, value_weight
    )
    edge_rows = passed_along(product[mix_rows - 2 :], "ep", 1)

    results = [None] * ep_count
    for number, (members, blocks) in enumerate(zip(chunks, arrived)):
        mine, other = spread(joined(blocks))
        with jax.named_scope(f"rows{number}"):
            keep, leave = expert_call(
                place, mine, other, expert_gain, expert_gate, expert_up, expert_down
            )
        summed = scattered(keep, leave, f"e{number}").reshape(len(blocks), block_rows, columns)
        with jax.named_scope(f"back{number}"):
            for j, s in enumerate(members):
                results[s] = swapped(summed[j], "ep", s) if s else summed[j]

    with jax.named_scope("rowsm"):
        keep, leave = output_call(
            lax.axis_size("tp") // 2, place, edge_rows, product, outer_gate, conv_weight, out_weight
        )
    mix_output = scattered(keep, leave, "m")

    normalized = route_weight / jnp.sum(route_weight, axis=1, keepdims=True) * routed_scale
    returned = jnp.concatenate(results, axis=0)
    total = 0.0
    for k, p in enumerate(picks):
        total = total + dot32(p.astype(jnp.bfloat16), returned) * normalized[:, k][:, None]
    return (mix_output, total.astype(jnp.bfloat16))


def solution(mesh):
    in_specs = (
        P("ep", "tp"),
        P(),
        P(None, "tp"),
        P(None, "tp"),
        P(None, "tp"),
        P(None, "tp"),
        P("tp", None),
        P("ep", "tp"),
        P(),
        P("ep", None),
        P("ep", None),
        P("ep", None, "tp"),
        P("ep", None, "tp"),
        P("ep", "tp", None),
    )
    out_specs = (P("ep", "tp"), P("ep", "tp"))
    return jax.shard_map(local, mesh=mesh, in_specs=in_specs, out_specs=out_specs, check_vma=False)
```

```python
import jax
import jax.numpy as jnp
from jax import lax
from jax.experimental import pallas as pl
from jax.experimental.pallas import tpu as pltpu
from jax.sharding import PartitionSpec as P

epsilon = 1e-06
routed_scale = 2.5


def passed_along(block, axis, distance):
    devices = range(lax.axis_size(axis))
    route = [(i - distance, i) for i in devices if i - distance in devices]
    return lax.ppermute(block, axis, route)


def swapped(block, axis, mask):
    return lax.ppermute(block, axis, [(i, i ^ mask) for i in range(lax.axis_size(axis))])


def spread(own):
    chips = lax.axis_size("tp") // 2
    mine = [own] + [swapped(own, "tp", 2 * s) for s in range(1, chips)]
    return mine, [swapped(block, "tp", 1) for block in mine]


def dot32(a, b):
    return jnp.dot(a, b, preferred_element_type=jnp.float32)


def column_start(place, distance, side, columns):
    chip = (place // 2) ^ distance
    return pl.multiple_of((2 * chip + (place % 2 if side == 0 else 1 - place % 2)) * columns, columns)


def assemble(place, mine, other, gain, scaled, factor):
    columns = mine[0].shape[1]
    squares = jnp.zeros(factor.shape, jnp.float32)
    for side, refs in enumerate((mine, other)):
        for distance, ref in enumerate(refs):
            at = pl.ds(column_start(place, distance, side, columns), columns)
            widened = ref[...].astype(jnp.float32)
            squares = squares + jnp.sum(widened * widened, axis=1, keepdims=True)
            scaled[:, at] = (widened * gain[:, at]).astype(jnp.bfloat16)
    factor[...] = lax.rsqrt(squares / scaled.shape[1] + epsilon)


def step_of(size):
    return 256 if size % 256 == 0 else size


def whole(shape):
    return pl.BlockSpec(shape, lambda *_: (0,) * len(shape))


def place_spec():
    return pl.BlockSpec(memory_space=pltpu.SMEM)


def expert_kernel(chips, place_ref, *refs):
    mine, other = refs[:chips], refs[chips : 2 * chips]
    gain, gate, up, down, keep, leave, scaled, factor, total = refs[2 * chips :]
    place = place_ref[0]
    step = pl.program_id(0)

    @pl.when(step == 0)
    def _():
        assemble(place, mine, other, gain, scaled, factor)

    hidden_gate = dot32(scaled[...], gate[0]) * factor[...]
    hidden_up = dot32(scaled[...], up[0]) * factor[...]
    activated = (hidden_gate / (1.0 + jnp.exp(-hidden_gate)) * hidden_up).astype(jnp.bfloat16)
    part = dot32(activated, down[0])

    @pl.when(step == 0)
    def _():
        total[...] = part

    @pl.when(step > 0)
    def _():
        total[...] += part

    @pl.when(step == pl.num_programs(0) - 1)
    def _():
        columns = keep.shape[2]
        for distance in range(chips):
            for side, out in enumerate((keep, leave)):
                at = pl.ds(column_start(place, distance, side, columns), columns)
                out[distance] = total[:, at].astype(jnp.bfloat16)


def expert_call(place, mine, other, gain, gate, up, down, room):
    chips = len(mine)
    rows, columns = mine[0].shape
    width, hidden = gate.shape[1:]
    step = step_of(hidden)
    out = jax.ShapeDtypeStruct((chips, rows, columns), jnp.bfloat16)
    return pl.pallas_call(
        lambda *refs: expert_kernel(chips, *refs),
        grid=(hidden // step,),
        in_specs=[place_spec()]
        + [whole((rows, columns))] * (2 * chips)
        + [
            whole((1, width)),
            pl.BlockSpec((1, width, step), lambda i: (0, 0, i)),
            pl.BlockSpec((1, width, step), lambda i: (0, 0, i)),
            pl.BlockSpec((1, step, width), lambda i: (0, i, 0)),
        ],
        out_specs=[whole(out.shape)] * 2,
        out_shape=[out] * 2,
        scratch_shapes=[
            pltpu.VMEM((rows, width), jnp.bfloat16),
            pltpu.VMEM((rows, 1), jnp.float32),
            pltpu.VMEM((rows, width), jnp.float32),
        ],
        cost_estimate=pl.CostEstimate(
            flops=6 * rows * width * hidden,
            bytes_accessed=6 * width * hidden,
            transcendentals=rows * hidden,
        ),
        compiler_params=pltpu.CompilerParams(vmem_limit_bytes=room * 2**20),
        name="expert_rows",
    )(place, *mine, *other, gain[None], gate, up, down)


def mixer_kernel(chips, place_ref, *refs):
    mine, other = refs[:chips], refs[chips : 2 * chips]
    gain, gate_b, gate_c, value, product, outer, scaled, factor = refs[2 * chips :]

    @pl.when(pl.program_id(0) == 0)
    def _():
        assemble(place_ref[0], mine, other, gain, scaled, factor)

    rows = scaled[...]
    product[...] = dot32(rows, gate_c[...]) * factor[...] * (dot32(rows, value[...]) * factor[...])
    outer[...] = dot32(rows, gate_b[...]) * factor[...]


def mixer_call(place, mine, other, gain, gate_b, gate_c, value):
    chips = len(mine)
    rows, columns = mine[0].shape
    width = gate_b.shape[0]
    step = step_of(columns)
    out = jax.ShapeDtypeStruct((rows, columns), jnp.float32)
    return pl.pallas_call(
        lambda *refs: mixer_kernel(chips, *refs),
        grid=(columns // step,),
        in_specs=[place_spec()]
        + [whole((rows, columns))] * (2 * chips)
        + [whole((1, width))]
        + [pl.BlockSpec((width, step), lambda i: (0, i))] * 3,
        out_specs=[pl.BlockSpec((rows, step), lambda i: (0, i))] * 2,
        out_shape=[out] * 2,
        scratch_shapes=[
            pltpu.VMEM((rows, width), jnp.bfloat16),
            pltpu.VMEM((rows, 1), jnp.float32),
        ],
        cost_estimate=pl.CostEstimate(
            flops=6 * rows * width * columns, bytes_accessed=6 * width * columns, transcendentals=0
        ),
        compiler_params=pltpu.CompilerParams(vmem_limit_bytes=22 * 2**20),
        name="mixer_rows",
    )(place, *mine, *other, gain[None], gate_b, gate_c, value)


def output_kernel(chips, place_ref, edge, product, outer, taps, weight, keep, leave):
    place = place_ref[0]
    now = product[...]
    row = lax.broadcasted_iota(jnp.int32, now.shape, 0)
    before = jnp.where(row == 0, edge[1:2], pltpu.roll(now, 1, 0))
    earlier = jnp.where(row == 0, edge[0:1], jnp.where(row == 1, edge[1:2], pltpu.roll(now, 2, 0)))
    convolved = taps[0:1] * earlier + taps[1:2] * before + taps[2:3] * now
    gated = (outer[...] * convolved).astype(jnp.bfloat16)
    columns = keep.shape[2]
    for distance in range(chips):
        for side, out in enumerate((keep, leave)):
            at = pl.ds(column_start(place, distance, side, columns), columns)
            out[distance] = dot32(gated, weight[:, at]).astype(jnp.bfloat16)


def output_call(chips, place, edge, product, outer, taps, weight):
    rows, columns = product.shape
    out = jax.ShapeDtypeStruct((chips, rows, columns), jnp.bfloat16)
    return pl.pallas_call(
        lambda *refs: output_kernel(chips, *refs),
        in_specs=[place_spec()] + [pl.BlockSpec(memory_space=pltpu.VMEM)] * 5,
        out_specs=[pl.BlockSpec(memory_space=pltpu.VMEM)] * 2,
        out_shape=[out] * 2,
        cost_estimate=pl.CostEstimate(
            flops=2 * rows * weight.shape[0] * weight.shape[1],
            bytes_accessed=2 * weight.shape[0] * weight.shape[1],
            transcendentals=0,
        ),
        compiler_params=pltpu.CompilerParams(vmem_limit_bytes=14 * 2**20),
        name="mixer_output",
    )(place, edge, product, outer, taps, weight)


def joined(blocks):
    rows, columns = blocks[0].shape
    if rows % 16:
        return jnp.concatenate(blocks, axis=0)

    def kernel(*refs):
        for j, ref in enumerate(refs[:-1]):
            refs[-1][j * rows : (j + 1) * rows] = ref[...]

    return pl.pallas_call(
        kernel,
        in_specs=[pl.BlockSpec(memory_space=pltpu.VMEM)] * len(blocks),
        out_specs=pl.BlockSpec(memory_space=pltpu.VMEM),
        out_shape=jax.ShapeDtypeStruct((rows * len(blocks), columns), blocks[0].dtype),
        compiler_params=pltpu.CompilerParams(vmem_limit_bytes=6 * 2**20),
        name="join_rows",
    )(*blocks)


def scattered(keep, leave):
    got = swapped(leave, "tp", 1)
    wide = [keep[s].astype(jnp.float32) + got[s].astype(jnp.float32) for s in range(keep.shape[0])]
    total = wide[0]
    for s in range(1, len(wide)):
        received = swapped(wide[s].astype(jnp.bfloat16), "tp", 2 * s)
        total = total + received.astype(jnp.float32)
    return total.astype(jnp.bfloat16)


def local(
    mix_input,
    mix_gain,
    gate_b_weight,
    gate_c_weight,
    value_weight,
    conv_weight,
    out_weight,
    expert_input,
    expert_gain,
    routes,
    route_weight,
    expert_gate,
    expert_up,
    expert_down,
):
    ep_count = lax.axis_size("ep")
    ep_me = lax.axis_index("ep")
    local_experts = expert_gate.shape[0]
    assert local_experts == 1
    expert_count = local_experts * ep_count
    tok_local, top_count = routes.shape
    capacity = 2 * tok_local * top_count // expert_count
    columns = expert_input.shape[1]
    mix_rows = mix_input.shape[0]
    block_rows = local_experts * capacity
    slots = ep_count * block_rows
    half = ep_count // 2

    place = lax.axis_index("tp").astype(jnp.int32)[None]
    mix_mine, mix_other = spread(mix_input)

    named = [routes[:, k][:, None] for k in range(top_count)]
    experts_iota = lax.broadcasted_iota(jnp.int32, (tok_local, expert_count), 1)
    hits = [(n == experts_iota) for n in named]
    any_hit = hits[0]
    for h in hits[1:]:
        any_hit = any_hit | h
    earlier = (
        lax.broadcasted_iota(jnp.int32, (tok_local, tok_local), 0)
        > lax.broadcasted_iota(jnp.int32, (tok_local, tok_local), 1)
    ).astype(jnp.bfloat16)
    counts = dot32(earlier, any_hit.astype(jnp.bfloat16)).astype(jnp.int32)
    slot_iota = lax.broadcasted_iota(jnp.int32, (tok_local, slots), 1)
    picks = []
    for n, h in zip(named, hits):
        rank = jnp.sum(jnp.where(h, counts, 0), axis=1, keepdims=True)
        index = (n // local_experts ^ ep_me) * block_rows + n % local_experts * capacity + rank
        picks.append(slot_iota == index)
    send = picks[0]
    for p in picks[1:]:
        send = send | p
    outgoing = lax.dot_general(
        send.astype(jnp.bfloat16),
        expert_input,
        (((0,), (0,)), ((), ())),
        preferred_element_type=jnp.float32,
    ).astype(jnp.bfloat16)
    outgoing = outgoing.reshape(ep_count, block_rows, columns)

    chunks = [range(half, ep_count), range(half)] if half else [range(ep_count)]
    arrived = []
    for members in chunks:
        arrived.append([swapped(outgoing[s], "ep", s) if s else outgoing[0] for s in members])

    product, outer_gate = mixer_call(
        place, mix_mine, mix_other, mix_gain, gate_b_weight, gate_c_weight, value_weight
    )
    edge_rows = passed_along(product[mix_rows - 2 :], "ep", 1)

    results = [None] * ep_count
    for number, (members, blocks) in enumerate(zip(chunks, arrived)):
        together = joined(blocks)
        mine, other = spread(together)
        keep, leave = expert_call(
            place, mine, other, expert_gain, expert_gate, expert_up, expert_down, 60 if number else 28
        )
        summed = scattered(keep, leave).reshape(len(blocks), block_rows, columns)
        for j, s in enumerate(members):
            results[s] = swapped(summed[j], "ep", s) if s else summed[j]

    keep, leave = output_call(
        lax.axis_size("tp") // 2, place, edge_rows, product, outer_gate, conv_weight, out_weight
    )
    mix_output = scattered(keep, leave)

    normalized = route_weight / jnp.sum(route_weight, axis=1, keepdims=True) * routed_scale
    returned = jnp.concatenate(results, axis=0)
    total = 0.0
    for k, p in enumerate(picks):
        total = total + dot32(p.astype(jnp.bfloat16), returned) * normalized[:, k][:, None]
    return (mix_output, total.astype(jnp.bfloat16))


def solution(mesh):
    in_specs = (
        P("ep", "tp"),
        P(),
        P(None, "tp"),
        P(None, "tp"),
        P(None, "tp"),
        P(None, "tp"),
        P("tp", None),
        P("ep", "tp"),
        P(),
        P("ep", None),
        P("ep", None),
        P("ep", None, "tp"),
        P("ep", None, "tp"),
        P("ep", "tp", None),
    )
    out_specs = (P("ep", "tp"), P("ep", "tp"))
    return jax.shard_map(local, mesh=mesh, in_specs=in_specs, out_specs=out_specs, check_vma=False)
```
